32 devices in a mesh: grp: 2 (over y), sp: 4 (over z), tp: 4 (over x, core).
Axes of the slice: x: 2, y: 2, z: 4, core: 2. Of those that a mesh axis runs over, the one named last changes fastest.
Arguments:
- resid: bfloat16 [4096, 2048], P(('grp', 'sp', 'tp')), parts along dimension 0, may hold values from -6 to 6
- pool_input: bfloat16 [4096, 512], P(('grp', 'sp'), 'tp'), parts along dimension 0, may hold values from -6 to 6
- group_map: bfloat16 [4, 128, 128], P('tp'), may hold values from -0.5 to 0.5
- pool_scale: bfloat16 [512], P('tp'), may hold values from 0.099609375 to 1.8984375
- out_proj: bfloat16 [512, 2048], P('tp'), may hold values from -0.25 to 0.25
- norm_gain: bfloat16 [2048], replicated, may hold values from 0.099609375 to 1.8984375
- routes: int32 [4096, 2], P(('grp', 'sp', 'tp')), parts along dimension 0, may hold values from 0 to 3, all different within a row; in each aligned block of 128 rows (0 to 127, 128 to 255, ...) at most 80 rows name the same one
- route_weight: float32 [4096, 2], P(('grp', 'sp', 'tp')), parts along dimension 0, may hold values from 0.2 to 1
- expert_gate: bfloat16 [4, 2048, 3584], P('sp', None, 'tp'), may hold values from -0.125 to 0.125
- expert_up: bfloat16 [4, 2048, 3584], P('sp', None, 'tp'), may hold values from -0.125 to 0.125
- expert_down: bfloat16 [4, 3584, 2048], P('sp', 'tp'), may hold values from -0.09375 to 0.09375
Outputs:
- layer_out: bfloat16 [4096, 2048], P(('grp', 'sp', 'tp')), parts along dimension 0
The draws below stay inside these ranges and needn't reach their ends.
There are 2 independent parts, one for each index of `grp`. The reference program is written for one: setup_inputs(seed, part) draws one part's arguments, and reference() takes and returns one part's arrays. A program takes and returns all parts, laid end to end along the dimension named above; an argument that names none is the same for every part. Nothing has to cross between parts.
Inputs may be any that keep to these rules, and one draw needn't show every extreme that they name: The 2 routes of a token differ. Among the tokens of one device (aligned blocks of 128 tokens), no expert is named more than 80 times, and in every draw some device names some expert exactly 80 times.
All inputs are finite; a program needn't handle non-finite values.
Results may differ from the reference program's by a relative error of at most 0.011.
Values may be sent and summed in bfloat16 or wider, within the bound.
A program may use at most 128 MiB of HBM per device.

```python
import math
import jax
import jax.numpy as jnp
import numpy as np
from jax import lax

D = 2048
GROUPS = 4
POOL_WIDTH = 512
GROUP_DIM = 128
EXPERT_FF = 3584
TOPK = 2
EXPERTS = 4
ROWS_DEV = 128
TOKENS = 2048
CAP = 80
N_SP = 4
N_TP = 4


def levels(key, dims, split, low, top_value):
    loudness = 1.0
    for position, blocks in split:
        steps = jax.random.uniform(jax.random.fold_in(jax.random.fold_in(key, 6), position), (blocks,), jnp.float32, low / len(split), top_value / len(split))
        loudness = loudness * jnp.repeat(jnp.exp(steps), dims[position] // blocks).reshape((-1,) + (1,) * (len(dims) - 1 - position))
    return loudness


def deal_out(own_key, own, number, rows, count, top, most, lean):
    sequence = jax.random.permutation(own_key, count)
    crowded, common = portions_of(count, rows * top, most, lean, True), portions_of(count, rows * top, most, lean, False)
    places = jnp.arange(count)

    def named(sizes, rotation):
        used = int((sizes > 0).sum())
        fixed = max(1, used // 4)
        shifted = fixed + (places - fixed + rotation * (used - fixed)) % max(1, count - fixed)
        return jnp.zeros((count,), jnp.int32).at[sequence[jnp.where(places < fixed, places, shifted)]].set(jnp.asarray(sizes, jnp.int32))

    sizes = jnp.where(number % 4 == 0, named(crowded, number // 4), named(common, number - number // 4 - 1))
    mixed = jax.random.permutation(jax.random.fold_in(own, 3), count)
    source_of, taker = mixed[0:count // 2 * 2:2], mixed[1:count // 2 * 2:2]
    slack = jnp.minimum(sizes[source_of] - 1, most - sizes[taker]) // 2
    slack = jnp.where((source_of == sequence[0]) | (taker == sequence[0]) | (sizes[taker] == 0), 0, jnp.maximum(slack, 0))
    shifted = jax.random.randint(jax.random.fold_in(own, 4), (count // 2,), 0, 1 << 20) % (slack + 1)
    sizes = sizes.at[source_of].add(-shifted).at[taker].add(shifted)
    members = jnp.searchsorted(jnp.cumsum(sizes), jnp.arange(rows * top), side="right").astype(jnp.int32)
    grid = members.reshape(top, rows).T
    grid = grid[jax.random.permutation(jax.random.fold_in(own, 1), rows)]
    rotation = jax.random.randint(jax.random.fold_in(own, 2), (rows, 1), 0, top)
    return jnp.take_along_axis(grid, (jnp.arange(top)[None, :] + rotation) % top, axis=1)


def portions_of(amount, total, reach, lean, full):
    portions = [(1 << 20) // math.isqrt(grade ** lean) + 1 for grade in range(1, amount + 1)]
    largest = reach if full else min(reach, max(-(-total // amount), total * portions[0] // sum(portions)))
    least = 1 if total - largest >= amount - 1 else 0
    counts, rest = [largest] + [least] * (amount - 1), total - largest - least * (amount - 1)
    while rest > 0:
        candidates = [i for i in range(1, amount) if counts[i] < largest] or [i for i in range(1, amount) if counts[i] < reach]
        mass, remaining = sum([portions[i] for i in candidates]), rest
        for i in candidates:
            more = min(reach - counts[i], max(1, remaining * portions[i] // mass), rest)
            counts[i] = counts[i] + more
            rest = rest - more
    return np.array(counts)


def bell_draw(key, shape, spread, limit, cuts=(), kind=jnp.bfloat16):
    result = spread * jax.random.normal(key, shape, jnp.float32)
    if cuts:
        result = result * levels(key, shape, cuts, -0.22, 0.18)
    return jnp.clip(result, -limit, limit).astype(kind)


def setup_inputs(seed: int = 0, part: int = 0) -> dict:
    keys = jax.random.split(jax.random.key(seed), 12)
    part_splits = jax.random.split(jax.random.fold_in(keys[11], part), 12)
    resid = bell_draw(part_splits[0], (TOKENS, D), 1.0, 6.0, ((0, 16),))
    pool_input = bell_draw(part_splits[1], (TOKENS, POOL_WIDTH), 1.0, 6.0, ((0, 4), (1, 4)))
    group_map = bell_draw(keys[2], (GROUPS, GROUP_DIM, GROUP_DIM), GROUP_DIM ** -0.5, 0.5, ((0, 4),))
    pool_scale = jnp.clip(1.0 + 0.18 * jax.random.normal(keys[3], (POOL_WIDTH,), jnp.float32), 0.099609375, 1.8984375).astype(jnp.bfloat16)
    out_proj = bell_draw(keys[4], (POOL_WIDTH, D), POOL_WIDTH ** -0.5, 0.25, ((0, 4),))
    norm_gain = jnp.clip(1.0 + 0.18 * jax.random.normal(keys[5], (D,), jnp.float32), 0.099609375, 1.8984375).astype(jnp.bfloat16)
    routes_keys = jax.random.split(jax.random.fold_in(part_splits[6], 1), TOKENS // ROWS_DEV)
    routes_turns = jax.random.permutation(jax.random.fold_in(part_splits[6], 3), TOKENS // ROWS_DEV)
    routes = jax.vmap(lambda own, number: deal_out(jax.random.fold_in(part_splits[6], 2), own, number, ROWS_DEV, EXPERTS, TOPK, CAP, 1))(routes_keys, routes_turns).reshape((TOKENS, TOPK))
    route_weight = jnp.clip(0.2 + 0.8 * jax.random.uniform(part_splits[7], (TOKENS, TOPK), jnp.float32) ** levels(part_splits[7], (TOKENS, TOPK), ((0, 16),), -0.2, 0.2), 0.2, 1.0)
    expert_gate = bell_draw(keys[8], (EXPERTS, D, EXPERT_FF), D ** -0.5, 0.125, ((0, 4), (2, 4)))
    expert_up = bell_draw(keys[9], (EXPERTS, D, EXPERT_FF), D ** -0.5, 0.125, ((0, 4), (2, 4)))
    expert_down = bell_draw(keys[10], (EXPERTS, EXPERT_FF, D), EXPERT_FF ** -0.5, 0.09375, ((0, 4), (1, 4)))
    return {"resid": resid, "pool_input": pool_input, "group_map": group_map, "pool_scale": pool_scale, "out_proj": out_proj, "norm_gain": norm_gain, "routes": routes, "route_weight": route_weight, "expert_gate": expert_gate, "expert_up": expert_up, "expert_down": expert_down}


norm_eps = 1e-06

def pool_group(values, window):
    window_sum = values
    for back in range(1, window):
        window_sum = window_sum + jnp.pad(values[:-back], ((back, 0), (0, 0)))
    divisor = jnp.minimum(jnp.arange(1, values.shape[0] + 1, dtype=jnp.float32), jnp.float32(window))
    return (window_sum / divisor[:, None] - values).astype(jnp.bfloat16)

def reference(resid, pool_input, group_map, pool_scale, out_proj, norm_gain, routes, route_weight, expert_gate, expert_up, expert_down):
    values = pool_input.astype(jnp.float32)
    pieces = []
    for group in range(GROUPS):
        low = group * GROUP_DIM
        pooled = pool_group(values[:, low:low + GROUP_DIM], 2 ** (group + 1))
        product = jnp.dot(pooled, group_map[group], preferred_element_type=jnp.float32)
        pieces.append((product * pool_scale[low:low + GROUP_DIM].astype(jnp.float32)).astype(jnp.bfloat16))
    group_out = jnp.concatenate(pieces, axis=1)
    mix = jnp.dot(group_out, out_proj, preferred_element_type=jnp.float32)
    mixed = (resid.astype(jnp.float32) + mix).astype(jnp.bfloat16)
    residual = mixed.astype(jnp.float32)
    scaled = residual * lax.rsqrt(lax.optimization_barrier(jnp.mean(residual * residual, axis=1, keepdims=True)) + norm_eps)
    normed = (scaled * norm_gain.astype(jnp.float32)).astype(jnp.bfloat16)
    flat_routes = routes.reshape(-1).astype(jnp.int32)
    flat_rows = jnp.repeat(normed, TOPK, axis=0)
    buffer_rows = N_SP * N_TP * CAP
    quarter = EXPERT_FF // N_TP

    def per_expert(carry, expert):
        chosen = flat_routes == expert
        rank = (jnp.cumsum(chosen.astype(jnp.int32)) - 1).astype(jnp.int32)
        place = jnp.where(chosen, rank, buffer_rows).astype(jnp.int32)
        buffer = jnp.zeros((buffer_rows, D), jnp.bfloat16).at[place].set(flat_rows, mode='drop')
        gate = jnp.dot(buffer, expert_gate[expert], preferred_element_type=jnp.float32)
        up_value = jnp.dot(buffer, expert_up[expert], preferred_element_type=jnp.float32)
        hidden = (jax.nn.silu(gate) * up_value).astype(jnp.bfloat16)
        down_w = expert_down[expert]
        output = jnp.zeros((buffer_rows, D), jnp.float32)
        for lane in range(N_TP):
            partial_out = jnp.dot(hidden[:, lane * quarter:(lane + 1) * quarter], down_w[lane * quarter:(lane + 1) * quarter], preferred_element_type=jnp.float32)
            output = output + lax.optimization_barrier(partial_out.astype(jnp.bfloat16)).astype(jnp.float32)
        picked = jnp.take(output, jnp.minimum(place, buffer_rows - 1), axis=0)
        return (carry + jnp.where(chosen[:, None], picked, jnp.float32(0.0)), None)
    routed, _ = lax.scan(per_expert, jnp.zeros((TOKENS * TOPK, D), jnp.float32), jnp.arange(EXPERTS, dtype=jnp.int32))
    moe = lax.optimization_barrier(jnp.sum(routed.reshape(TOKENS, TOPK, D) * route_weight.astype(jnp.float32)[:, :, None], axis=1))
    return (residual + moe).astype(jnp.bfloat16)
```

```python
import functools

import jax
import jax.numpy as jnp
from jax import lax
from jax.experimental import pallas as pl
from jax.experimental.pallas import tpu as pltpu
from jax.sharding import PartitionSpec as P

GROUPS = 4
norm_eps = 1e-06
BF = jnp.bfloat16
F32 = jnp.float32
MESH = pl.DeviceIdType.MESH
RIM = 2**GROUPS


def offset(j):
    half = (j + 1) // 2
    return half * (2 * lax.rem(j, 2) - 1)


def kernel(
    S, T, R, SL,
    resid, pool, gmap, scale, oproj, gain, routes, routes_t, weight, wg, wu, wd,
    out,
    wgu_v, wd_v, opj, rim, piece, gout, stage, inbox, pbuf, rbuf, fbuf, fin, ret,
    acc, hid, mixed_v, normed_v,
    w_sem, o_far_s, o_far_r, o_near_s, o_near_r, rim_s, rim_r, pc_s, pc_r,
    z_s, z_r, f_s, f_r, n_s, n_r, pn_s, pn_r, pf_s, pf_r, rz_s, rz_r,
):
    s = lax.axis_index("sp")
    t = lax.axis_index("tp")
    H = T // 2
    D = resid.shape[1]
    F = wd.shape[0]
    near = t + 1 - 2 * lax.rem(t, 2)

    def up(k):
        return lax.rem(t + 2 * k, T)

    def down(base, k):
        return lax.rem(base - 2 * k + 2 * T, T)

    def remote(src, dst, ss, rs, sp=None, tp=None):
        return pltpu.make_async_remote_copy(
            src_ref=src, dst_ref=dst, send_sem=ss, recv_sem=rs,
            device_id={"sp": s if sp is None else sp, "tp": t if tp is None else tp},
            device_id_type=MESH,
        )

    loads = [
        pltpu.make_async_copy(wg, wgu_v.at[:, pl.ds(0, F)], w_sem.at[0]),
        pltpu.make_async_copy(wu, wgu_v.at[:, pl.ds(F, F)], w_sem.at[1]),
        pltpu.make_async_copy(wd, wd_v, w_sem.at[2]),
    ]
    for load in loads:
        load.start()

    barrier = pltpu.get_barrier_semaphore()

    @pl.loop(1, S)
    def _(j):
        pl.semaphore_signal(
            barrier, inc=1, device_id={"sp": lax.rem(s + j, S), "tp": t}, device_id_type=MESH
        )

    for j in range(1, T):
        pl.semaphore_signal(
            barrier, inc=1, device_id={"sp": s, "tp": lax.rem(t + j, T)}, device_id_type=MESH
        )
    pl.semaphore_wait(barrier, S - 1 + T - 1)

    seq = pool.shape[0]
    rim_copy = remote(
        pool.at[pl.ds(seq - RIM, RIM)], rim, rim_s.at[0], rim_r.at[0], sp=lax.rem(s + 1, S)
    )
    rim_copy.start()

    def o_far(k):
        return remote(oproj, opj.at[t], o_far_s.at[k], o_far_r.at[k], tp=up(k))

    def o_near(k):
        block = down(t, k)
        return remote(
            oproj if k == 0 else opj.at[block], opj.at[block], o_near_s.at[k], o_near_r.at[k],
            tp=near,
        )

    for k in range(1, H):
        o_far(k).start()
    o_near(0).start()

    E = S
    EP = max(8, E)
    e_row = lax.broadcasted_iota(jnp.int32, (EP, R), 0)
    hot_row = [e_row == routes_t[k : k + 1, :] for k in range(2)]
    both_row = jnp.where(hot_row[0] | hot_row[1], 1.0, 0.0).astype(BF)
    before = lax.broadcasted_iota(jnp.int32, (R, R), 0) < lax.broadcasted_iota(
        jnp.int32, (R, R), 1
    )
    rank_row = jnp.dot(both_row, jnp.where(before, 1.0, 0.0).astype(BF), preferred_element_type=F32)
    slot_row = rank_row + (e_row * SL).astype(F32)
    tgt_row = [jnp.sum(jnp.where(h, slot_row, 0.0), axis=0, keepdims=True) for h in hot_row]

    EL = 128
    e_col = lax.broadcasted_iota(jnp.int32, (R, EL), 1)
    hot_col = [e_col == routes[:, k : k + 1] for k in range(2)]
    both_col = jnp.where(hot_col[0] | hot_col[1], 1.0, 0.0).astype(BF)
    after = lax.broadcasted_iota(jnp.int32, (R, R), 1) < lax.broadcasted_iota(
        jnp.int32, (R, R), 0
    )
    rank_col = jnp.dot(jnp.where(after, 1.0, 0.0).astype(BF), both_col, preferred_element_type=F32)
    slot_col = rank_col + (e_col * SL).astype(F32)
    tgt_col = [jnp.sum(jnp.where(h, slot_col, 0.0), axis=1, keepdims=True) for h in hot_col]

    rim_copy.wait_recv()
    values = pool[...].astype(F32)
    rim_v = jnp.where(s > 0, rim[...].astype(F32), 0.0)
    run = jnp.concatenate([rim_v, values], axis=0)
    window_sum = None
    for g in range(GROUPS):
        run = run + pltpu.roll(run, 2**g, 0)
        part = run[RIM:]
        window_sum = part if g == 0 else jnp.where(t >= g, part, window_sum)
    window = jnp.int32(2)
    for g in range(1, GROUPS):
        window = jnp.where(t >= g, jnp.int32(2 ** (g + 1)), window)
    position = s * seq + 1 + lax.broadcasted_iota(jnp.int32, (seq, 128), 0)
    divisor = jnp.minimum(position, window).astype(F32)
    pooled = (window_sum / divisor - values).astype(BF)
    product = jnp.dot(pooled, gmap[0], preferred_element_type=F32)
    piece[...] = (product * scale[...].astype(F32)).astype(BF).reshape(T, R, 128)

    def piece_copy(j):
        q = lax.rem(t + j, T)
        return remote(piece.at[q], gout.at[t], pc_s.at[j], pc_r.at[j], tp=q)

    for j in range(1, T):
        piece_copy(j).start()

    for k in range(1, H):
        o_far(k).wait_recv()
        o_near(k).start()

    for j in range(1, T):
        piece_copy(j).wait_recv()
    for k in range(H):
        o_near(k).wait_recv()

    gout[t] = piece[t]
    opj[t] = oproj[...]
    mix = resid[...].astype(F32)
    total = jnp.dot(gout[0], opj[0], preferred_element_type=F32)
    for q in range(1, T):
        total = total + jnp.dot(gout[q], opj[q], preferred_element_type=F32)
    mixed = (mix + total).astype(BF)
    mixed_v[...] = mixed
    residual = mixed.astype(F32)
    scaled = residual * lax.rsqrt(jnp.mean(residual * residual, axis=1, keepdims=True) + norm_eps)
    normed_v[...] = (scaled * gain[...].astype(F32)).astype(BF)

    slot_iota = lax.broadcasted_iota(jnp.int32, (SL, R), 0)

    def rows_of(e):
        want = (slot_iota + e * SL).astype(F32)
        place = jnp.where((tgt_row[0] == want) | (tgt_row[1] == want), 1.0, 0.0).astype(BF)
        return jnp.dot(place, normed_v[...], preferred_element_type=F32).astype(BF)

    def dest(j):
        return lax.rem(s + offset(j) + S, S)

    def source(j):
        return lax.rem(s - offset(j) + S, S)

    def z_copy(j):
        return remote(stage.at[j], inbox.at[s, t], z_s.at[j], z_r.at[j], sp=dest(j))

    def far_copy(j, k):
        block = inbox.at[source(j), t]
        return remote(block, block, f_s.at[j, k], f_r.at[j, k], tp=up(k))

    def near_copy(j, k):
        block = inbox.at[source(j), down(t, k)]
        return remote(block, block, n_s.at[j, k], n_r.at[j, k], tp=near)

    def forward_own(j):
        for k in range(1, H):
            far_copy(j, k).start()
        near_copy(j, 0).start()

    def p_near(j, k):
        return remote(
            pbuf.at[j, down(near, k)], rbuf.at[j, k], pn_s.at[j, k], pn_r.at[j, k], tp=near
        )

    def p_far(j, k):
        q = down(t, k)
        return remote(pbuf.at[j, q], fbuf.at[j, k], pf_s.at[j, k], pf_r.at[j, k], tp=q)

    def back(j):
        return remote(fin.at[j], ret.at[s], rz_s.at[j], rz_r.at[j], sp=source(j))

    inbox[s, t] = rows_of(s)
    forward_own(0)

    @pl.loop(1, S)
    def _(j):
        stage[j] = rows_of(dest(j))
        z_copy(j).start()

    for load in loads:
        load.wait()

    def arrive(j):
        z_copy(j).wait_recv()
        forward_own(j)

    if S > 1:
        arrive(1)

    NT = 256 if (2 * F) % 256 == 0 else 128
    DT = 256 if D % 256 == 0 else 128

    @pl.loop(0, S + 2)
    def _(j):
        @pl.when(j + 2 < S)
        def _():
            arrive(j + 2)

        @pl.when((j >= 1) & (j <= S))
        def _():
            i = j - 1
            for k in range(H):
                p_near(i, k).wait_recv()
            for k in range(1, H):
                q = down(t, k)
                pbuf[i, q] = (pbuf[i, q].astype(F32) + rbuf[i, k].astype(F32)).astype(BF)
                p_far(i, k).start()

        @pl.when(j < S)
        def _():
            for k in range(1, H):
                far_copy(j, k).wait_recv()
                near_copy(j, k).start()

        @pl.when(j >= 2)
        def _():
            i = j - 2
            value = pbuf[i, t].astype(F32) + rbuf[i, 0].astype(F32)
            for k in range(1, H):
                p_far(i, k).wait_recv()
                value = value + fbuf[i, k].astype(F32)
            fin[i] = value.astype(BF)

            @pl.when(i > 0)
            def _():
                back(i).start()

        @pl.when(j < S)
        def _():
            for k in range(H):
                near_copy(j, k).wait_recv()
            src = source(j)

            @pl.loop(0, 2 * F // NT)
            def _(n):
                cols = pl.ds(pl.multiple_of(n * NT, NT), NT)
                x = inbox[src].reshape(T * SL, D)
                acc[:, cols] = jnp.dot(x, wgu_v[:, cols], preferred_element_type=F32)

            gate = acc[:, :F]
            hid[...] = (gate / (1.0 + jnp.exp(-gate)) * acc[:, F:]).astype(BF)

            @pl.loop(0, D // DT)
            def _(n):
                cols = pl.ds(pl.multiple_of(n * DT, DT), DT)
                y = jnp.dot(hid[...], wd_v[:, cols], preferred_element_type=F32)
                pbuf[j, :, :, cols] = y.astype(BF).reshape(T, SL, DT)

            for k in range(H):
                p_near(j, k).start()

    @pl.loop(1, S)
    def _(j):
        back(j).wait_recv()

    ret[s] = fin[0]
    flat = ret[...].reshape(S * SL, D)
    lanes = lax.broadcasted_iota(jnp.int32, (R, S * SL), 1).astype(F32)
    total = mixed_v[...].astype(F32)
    picked = [
        weight[:, k : k + 1]
        * jnp.dot(
            jnp.where(tgt_col[k] == lanes, 1.0, 0.0).astype(BF), flat, preferred_element_type=F32
        )
        for k in range(2)
    ]
    out[...] = (total + (picked[0] + picked[1])).astype(BF)

    rim_copy.wait_send()
    for k in range(1, H):
        o_far(k).wait_send()
    for k in range(H):
        o_near(k).wait_send()
    for j in range(1, T):
        piece_copy(j).wait_send()

    @pl.loop(0, S)
    def _(j):
        for k in range(1, H):
            far_copy(j, k).wait_send()
            p_far(j, k).wait_send()
        for k in range(H):
            near_copy(j, k).wait_send()
            p_near(j, k).wait_send()

    @pl.loop(1, S)
    def _(j):
        z_copy(j).wait_send()
        back(j).wait_send()


def local(
    resid, pool_input, group_map, pool_scale, out_proj, norm_gain, routes, route_weight,
    expert_gate, expert_up, expert_down,
):
    S, T = lax.axis_size("sp"), lax.axis_size("tp")
    R, D = resid.shape
    H = T // 2
    top = routes.shape[1]
    experts = S * expert_gate.shape[0]
    slots = max(2, 5 * R * top // (4 * experts))
    SL = -(-slots // 16) * 16
    F = expert_down.shape[1]
    GD = group_map.shape[1]
    vmem, hbm = pl.BlockSpec(memory_space=pltpu.VMEM), pl.BlockSpec(memory_space=pl.ANY)
    dma = lambda *n: pltpu.SemaphoreType.DMA(n)
    buf = lambda *n: pltpu.VMEM(n, BF)
    return pl.pallas_call(
        functools.partial(kernel, S, T, R, SL),
        out_shape=jax.ShapeDtypeStruct((R, D), BF),
        in_specs=[vmem] * 9 + [hbm] * 3,
        out_specs=vmem,
        scratch_shapes=[
            buf(D, 2 * F), buf(F, D), buf(T, GD, D), buf(RIM, GD), buf(T, R, GD), buf(T, R, GD),
            buf(S, SL, D), buf(S, T, SL, D), buf(S, T, SL, D), buf(S, H, SL, D), buf(S, H, SL, D),
            buf(S, SL, D), buf(S, SL, D),
            pltpu.VMEM((T * SL, 2 * F), F32), buf(T * SL, F), buf(R, D), buf(R, D),
            dma(3), dma(H), dma(H), dma(H), dma(H), dma(1), dma(1), dma(T), dma(T),
            dma(S), dma(S), dma(S, H), dma(S, H), dma(S, H), dma(S, H),
            dma(S, H), dma(S, H), dma(S, H), dma(S, H), dma(S), dma(S),
        ],
        compiler_params=pltpu.CompilerParams(
            collective_id=0, has_side_effects=True, vmem_limit_bytes=63 * 1024 * 1024
        ),
    )(
        resid, pool_input, group_map, pool_scale.reshape(1, -1), out_proj,
        norm_gain.reshape(1, -1), routes, routes.T, route_weight,
        expert_gate[0], expert_up[0], expert_down[0],
    )


def solution(mesh):
    return jax.shard_map(
        local,
        mesh=mesh,
        in_specs=(
            P(("grp", "sp", "tp"), None),
            P(("grp", "sp"), "tp"),
            P("tp", None, None),
            P("tp"),
            P("tp", None),
            P(),
            P(("grp", "sp", "tp"), None),
            P(("grp", "sp", "tp"), None),
            P("sp", None, "tp"),
            P("sp", None, "tp"),
            P("sp", "tp", None),
        ),
        out_specs=P(("grp", "sp", "tp"), None),
        check_vma=False,
    )
```

```python
import functools

import jax
import jax.numpy as jnp
from jax import lax
from jax.experimental import pallas as pl
from jax.experimental.pallas import tpu as pltpu
from jax.sharding import PartitionSpec as P

GROUPS = 4
norm_eps = 1e-06
BF = jnp.bfloat16
F32 = jnp.float32
MESH = pl.DeviceIdType.MESH
RIM = 2**GROUPS


def nearest(s, j, S):
    low = jnp.minimum(s, S - 1 - s)
    half = (j + 1) // 2
    both = half * (2 * lax.rem(j, 2) - 1)
    rest = (j - low) * (1 - 2 * ((2 * s) // S))
    return s + jnp.where(j <= 2 * low, both * (1 - 2 * ((2 * s) // S)), rest)


def kernel(
    S, T, R, SL,
    resid, pool, gmap, scale, oproj, gain, routes_t, weight_t, wg, wu, wd,
    out,
    wgu_v, wd_v, opj, rim, piece, gout, stage, inbox, pbuf, rbuf, fbuf, fin, ret,
    acc, hid, mixed_v, normed_v,
    w_sem, o_far_s, o_far_r, o_near_s, o_near_r, rim_s, rim_r, pc_s, pc_r,
    z_s, z_r, f_s, f_r, n_s, n_r, pn_s, pn_r, pf_s, pf_r, rz_s, rz_r,
):
    s = lax.axis_index("sp")
    t = lax.axis_index("tp")
    H = T // 2
    D = resid.shape[1]
    F = wd.shape[0]
    near = t + 1 - 2 * lax.rem(t, 2)

    def up(k):
        return lax.rem(t + 2 * k, T)

    def down(base, k):
        return lax.rem(base - 2 * k + 2 * T, T)

    def remote(src, dst, ss, rs, sp=None, tp=None):
        return pltpu.make_async_remote_copy(
            src_ref=src, dst_ref=dst, send_sem=ss, recv_sem=rs,
            device_id={"sp": s if sp is None else sp, "tp": t if tp is None else tp},
            device_id_type=MESH,
        )

    loads = [
        pltpu.make_async_copy(wg, wgu_v.at[:, pl.ds(0, F)], w_sem.at[0]),
        pltpu.make_async_copy(wu, wgu_v.at[:, pl.ds(F, F)], w_sem.at[1]),
        pltpu.make_async_copy(wd, wd_v, w_sem.at[2]),
    ]
    for load in loads:
        load.start()

    barrier = pltpu.get_barrier_semaphore()

    @pl.loop(1, S)
    def _(j):
        pl.semaphore_signal(
            barrier, inc=1, device_id={"sp": lax.rem(s + j, S), "tp": t}, device_id_type=MESH
        )

    for j in range(1, T):
        pl.semaphore_signal(
            barrier, inc=1, device_id={"sp": s, "tp": lax.rem(t + j, T)}, device_id_type=MESH
        )
    pl.semaphore_wait(barrier, S - 1 + T - 1)

    seq = pool.shape[0]
    rim_copy = remote(
        pool.at[pl.ds(seq - RIM, RIM)], rim, rim_s.at[0], rim_r.at[0], sp=lax.rem(s + 1, S)
    )
    rim_copy.start()

    def o_far(k):
        return remote(oproj, opj.at[t], o_far_s.at[k], o_far_r.at[k], tp=up(k))

    def o_near(k):
        block = down(t, k)
        return remote(
            oproj if k == 0 else opj.at[block], opj.at[block], o_near_s.at[k], o_near_r.at[k],
            tp=near,
        )

    for k in range(1, H):
        o_far(k).start()
    o_near(0).start()

    E = S
    EP = max(8, E)
    e_row = lax.broadcasted_iota(jnp.int32, (EP, R), 0)
    hot_row = [e_row == routes_t[k : k + 1, :] for k in range(2)]
    both_row = jnp.where(hot_row[0] | hot_row[1], 1.0, 0.0).astype(BF)
    before = lax.broadcasted_iota(jnp.int32, (R, R), 0) < lax.broadcasted_iota(
        jnp.int32, (R, R), 1
    )
    rank_row = jnp.dot(both_row, jnp.where(before, 1.0, 0.0).astype(BF), preferred_element_type=F32)
    slot_row = rank_row + (e_row * SL).astype(F32)
    tgt_row = [jnp.sum(jnp.where(h, slot_row, 0.0), axis=0, keepdims=True) for h in hot_row]

    eye = lax.broadcasted_iota(jnp.int32, (R, R), 0) == lax.broadcasted_iota(
        jnp.int32, (R, R), 1
    )

    def column(row):
        return jnp.sum(jnp.where(eye, row, 0.0), axis=1, keepdims=True)

    tgt_col = [column(row) for row in tgt_row]
    weight_col = [column(weight_t[k : k + 1, :]) for k in range(2)]

    rim_copy.wait_recv()
    values = pool[...].astype(F32)
    rim_v = jnp.where(s > 0, rim[...].astype(F32), 0.0)
    run = jnp.concatenate([rim_v, values], axis=0)
    window_sum = None
    for g in range(GROUPS):
        run = run + pltpu.roll(run, 2**g, 0)
        part = run[RIM:]
        window_sum = part if g == 0 else jnp.where(t >= g, part, window_sum)
    window = jnp.int32(2)
    for g in range(1, GROUPS):
        window = jnp.where(t >= g, jnp.int32(2 ** (g + 1)), window)
    position = s * seq + 1 + lax.broadcasted_iota(jnp.int32, (seq, 128), 0)
    divisor = jnp.minimum(position, window).astype(F32)
    pooled = (window_sum / divisor - values).astype(BF)
    product = jnp.dot(pooled, gmap[0], preferred_element_type=F32)
    piece[...] = (product * scale[...].astype(F32)).astype(BF).reshape(T, R, 128)

    def piece_copy(j):
        q = lax.rem(t + j, T)
        return remote(piece.at[q], gout.at[t], pc_s.at[j], pc_r.at[j], tp=q)

    for j in range(1, T):
        piece_copy(j).start()

    for k in range(1, H):
        o_far(k).wait_recv()
        o_near(k).start()

    for j in range(1, T):
        piece_copy(j).wait_recv()
    for k in range(H):
        o_near(k).wait_recv()

    gout[t] = piece[t]
    opj[t] = oproj[...]
    mix = resid[...].astype(F32)
    total = jnp.dot(gout[0], opj[0], preferred_element_type=F32)
    for q in range(1, T):
        total = total + jnp.dot(gout[q], opj[q], preferred_element_type=F32)
    mixed = (mix + total).astype(BF)
    mixed_v[...] = mixed
    residual = mixed.astype(F32)
    scaled = residual * lax.rsqrt(jnp.mean(residual * residual, axis=1, keepdims=True) + norm_eps)
    normed_v[...] = (scaled * gain[...].astype(F32).reshape(1, D)).astype(BF)

    slot_iota = lax.broadcasted_iota(jnp.int32, (SL, R), 0)

    def rows_of(e):
        want = (slot_iota + e * SL).astype(F32)
        place = jnp.where((tgt_row[0] == want) | (tgt_row[1] == want), 1.0, 0.0).astype(BF)
        return jnp.dot(place, normed_v[...], preferred_element_type=F32).astype(BF)

    def dest(j):
        return nearest(s, S - j, S)

    def source(j):
        return nearest(s, lax.rem(S - j, S), S)

    def z_copy(e):
        return remote(stage.at[e], inbox.at[s, t], z_s.at[e], z_r.at[s], sp=e)

    def z_arrival(i):
        return remote(stage.at[i], inbox.at[i, t], z_s.at[i], z_r.at[i], sp=i)

    def far_copy(j, k):
        block = inbox.at[source(j), t]
        return remote(block, block, f_s.at[j, k], f_r.at[j, k], tp=up(k))

    def near_copy(j, k):
        block = inbox.at[source(j), down(t, k)]
        return remote(block, block, n_s.at[j, k], n_r.at[j, k], tp=near)

    def forward_own(j):
        for k in range(1, H):
            far_copy(j, k).start()
        near_copy(j, 0).start()

    def p_near(j, k):
        return remote(
            pbuf.at[j, down(near, k)], rbuf.at[j, k], pn_s.at[j, k], pn_r.at[j, k], tp=near
        )

    def p_far(j, k):
        q = down(t, k)
        return remote(pbuf.at[j, q], fbuf.at[j, k], pf_s.at[j, k], pf_r.at[j, k], tp=q)

    def back(j):
        return remote(fin.at[j], ret.at[s], rz_s.at[j], rz_r.at[s], sp=source(j))

    def back_arrival(j):
        e = source(j)
        return remote(fin.at[j], ret.at[e], rz_s.at[j], rz_r.at[e], sp=e)

    inbox[s, t] = rows_of(s)
    forward_own(0)

    @pl.loop(1, S)
    def _(j):
        e = dest(j)
        stage[e] = rows_of(e)
        z_copy(e).start()

    for load in loads:
        load.wait()

    def arrive(j):
        z_arrival(source(j)).wait_recv()
        forward_own(j)

    NT = 256 if (2 * F) % 256 == 0 else 128
    DT = 256 if D % 256 == 0 else 128

    @pl.loop(0, S + 2)
    def _(j):
        @pl.when((j + 1 < S) & (j + 1 > 0))
        def _():
            arrive(j + 1)

        @pl.when((j >= 1) & (j <= S))
        def _():
            i = j - 1
            for k in range(H):
                p_near(i, k).wait_recv()
            for k in range(1, H):
                q = down(t, k)
                pbuf[i, q] = (pbuf[i, q].astype(F32) + rbuf[i, k].astype(F32)).astype(BF)
                p_far(i, k).start()

        @pl.when(j < S)
        def _():
            for k in range(1, H):
                far_copy(j, k).wait_recv()
                near_copy(j, k).start()

        @pl.when(j >= 2)
        def _():
            i = j - 2
            value = pbuf[i, t].astype(F32) + rbuf[i, 0].astype(F32)
            for k in range(1, H):
                p_far(i, k).wait_recv()
                value = value + fbuf[i, k].astype(F32)
            fin[i] = value.astype(BF)

            @pl.when(i > 0)
            def _():
                back(i).start()

        @pl.when(j < S)
        def _():
            for k in range(H):
                near_copy(j, k).wait_recv()
            src = source(j)

            @pl.loop(0, 2 * F // NT)
            def _(n):
                cols = pl.ds(pl.multiple_of(n * NT, NT), NT)
                x = inbox[src].reshape(T * SL, D)
                acc[:, cols] = jnp.dot(x, wgu_v[:, cols], preferred_element_type=F32)

            gate = acc[:, :F]
            hid[...] = (gate / (1.0 + jnp.exp(-gate)) * acc[:, F:]).astype(BF)

            @pl.loop(0, D // DT)
            def _(n):
                cols = pl.ds(pl.multiple_of(n * DT, DT), DT)
                y = jnp.dot(hid[...], wd_v[:, cols], preferred_element_type=F32)
                pbuf[j, :, :, cols] = y.astype(BF).reshape(T, SL, DT)

            for k in range(H):
                p_near(j, k).start()

    @pl.loop(1, S)
    def _(j):
        back_arrival(j).wait_recv()

    ret[s] = fin[0]
    flat = ret[...].reshape(S * SL, D)
    lanes = lax.broadcasted_iota(jnp.int32, (R, S * SL), 1).astype(F32)
    total = mixed_v[...].astype(F32)
    picked = [
        weight_col[k]
        * jnp.dot(
            jnp.where(tgt_col[k] == lanes, 1.0, 0.0).astype(BF), flat, preferred_element_type=F32
        )
        for k in range(2)
    ]
    out[...] = (total + (picked[0] + picked[1])).astype(BF)

    rim_copy.wait_send()
    for k in range(1, H):
        o_far(k).wait_send()
    for k in range(H):
        o_near(k).wait_send()
    for j in range(1, T):
        piece_copy(j).wait_send()

    @pl.loop(0, S)
    def _(j):
        for k in range(1, H):
            far_copy(j, k).wait_send()
            p_far(j, k).wait_send()
        for k in range(H):
            near_copy(j, k).wait_send()
            p_near(j, k).wait_send()

    @pl.loop(1, S)
    def _(j):
        z_copy(dest(j)).wait_send()
        back(j).wait_send()


def local(
    resid, pool_input, group_map, pool_scale, out_proj, norm_gain, routes, route_weight,
    expert_gate, expert_up, expert_down,
):
    S, T = lax.axis_size("sp"), lax.axis_size("tp")
    R, D = resid.shape
    H = T // 2
    top = routes.shape[1]
    experts = S * expert_gate.shape[0]
    slots = max(2, 5 * R * top // (4 * experts))
    SL = -(-slots // 16) * 16
    F = expert_down.shape[1]
    GD = group_map.shape[1]
    vmem, hbm = pl.BlockSpec(memory_space=pltpu.VMEM), pl.BlockSpec(memory_space=pl.ANY)
    dma = lambda *n: pltpu.SemaphoreType.DMA(n)
    buf = lambda *n: pltpu.VMEM(n, BF)
    return pl.pallas_call(
        functools.partial(kernel, S, T, R, SL),
        out_shape=jax.ShapeDtypeStruct((R, D), BF),
        in_specs=[vmem] * 8 + [hbm] * 3,
        out_specs=vmem,
        scratch_shapes=[
            buf(D, 2 * F), buf(F, D), buf(T, GD, D), buf(RIM, GD), buf(T, R, GD), buf(T, R, GD),
            buf(S, SL, D), buf(S, T, SL, D), buf(S, T, SL, D), buf(S, H, SL, D), buf(S, H, SL, D),
            buf(S, SL, D), buf(S, SL, D),
            pltpu.VMEM((T * SL, 2 * F), F32), buf(T * SL, F), buf(R, D), buf(R, D),
            dma(3), dma(H), dma(H), dma(H), dma(H), dma(1), dma(1), dma(T), dma(T),
            dma(S), dma(S), dma(S, H), dma(S, H), dma(S, H), dma(S, H),
            dma(S, H), dma(S, H), dma(S, H), dma(S, H), dma(S), dma(S),
        ],
        compiler_params=pltpu.CompilerParams(
            collective_id=0, has_side_effects=True, vmem_limit_bytes=63 * 1024 * 1024
        ),
    )(
        resid, pool_input, group_map, pool_scale.reshape(1, -1), out_proj,
        norm_gain, routes.T, route_weight.T,
        expert_gate[0], expert_up[0], expert_down[0],
    )


def solution(mesh):
    return jax.shard_map(
        local,
        mesh=mesh,
        in_specs=(
            P(("grp", "sp", "tp"), None),
            P(("grp", "sp"), "tp"),
            P("tp", None, None),
            P("tp"),
            P("tp", None),
            P(),
            P(("grp", "sp", "tp"), None),
            P(("grp", "sp", "tp"), None),
            P("sp", None, "tp"),
            P("sp", None, "tp"),
            P("sp", "tp", None),
        ),
        out_specs=P(("grp", "sp", "tp"), None),
        check_vma=False,
    )
```
